32 devices in a mesh: ep: 16 (over z, y, x), tp: 2 (over core).
Axes of the slice: x: 2, y: 2, z: 4, core: 2. Of those that a mesh axis runs over, the one named last changes fastest.
Arguments:
- hidden: bfloat16 [1024, 2048], P('ep'), may hold values from -6 to 6
- mix_gain: float32 [2048], replicated, may hold values from 0.1 to 1.9
- recept_weight: bfloat16 [2048, 1024], P(None, 'tp'), may hold values from -0.125 to 0.125
- key_weight: bfloat16 [2048, 1024], P(None, 'tp'), may hold values from -0.125 to 0.125
- value_weight: bfloat16 [2048, 1024], P(None, 'tp'), may hold values from -0.125 to 0.125
- decay_down: bfloat16 [2048, 64], replicated, may hold values from -0.125 to 0.125
- decay_up: bfloat16 [64, 1024], replicated, may hold values from -0.75 to 0.75
- decay_bias: float32 [1024], replicated, may hold values from -4 to 1
- rate_down: bfloat16 [2048, 64], replicated, may hold values from -0.125 to 0.125
- rate_up: bfloat16 [64, 1024], replicated, may hold values from -0.75 to 0.75
- rate_bias: float32 [1024], replicated, may hold values from -4 to 4
- head_gain: float32 [1024], replicated, may hold values from 0.1 to 1.9
- out_weight: bfloat16 [1024, 2048], P('tp'), may hold values from -0.1875 to 0.1875
- memory_state: float32 [1024, 16, 64, 64], P('ep', 'tp'), may hold values from -6 to 6
- ffn_gain: float32 [2048], replicated, may hold values from 0.1 to 1.9
- blend_vector: bfloat16 [2048], replicated, may hold values from -0.125 to 0.125
- dense_gate: bfloat16 [2048, 5632], P(None, ('ep', 'tp')), may hold values from -0.125 to 0.125
- dense_up: bfloat16 [2048, 5632], P(None, ('ep', 'tp')), may hold values from -0.125 to 0.125
- dense_down: bfloat16 [5632, 2048], P(('ep', 'tp')), may hold values from -0.3125 to 0.3125
- expert_gate: bfloat16 [16, 2048, 1536], P('ep', None, 'tp'), may hold values from -0.125 to 0.125
- expert_up: bfloat16 [16, 2048, 1536], P('ep', None, 'tp'), may hold values from -0.125 to 0.125
- expert_down: bfloat16 [16, 1536, 2048], P('ep', 'tp'), may hold values from -0.15625 to 0.15625
- routing: int32 [1024, 2], P('ep'), may hold values from 0 to 15, all different within a row; in each aligned block of 64 rows (0 to 63, 64 to 127, ...) at most 16 rows name the same one
- route_scale: float32 [1024, 2], P('ep'), may hold values from 0.25 to 1
Outputs:
- layer_out: bfloat16 [1024, 2048], P('ep')
- new_state: float32 [1024, 16, 64, 64], P('ep', 'tp')
The draws below stay inside these ranges and needn't reach their ends.
Inputs may be any that keep to these rules, and one draw needn't show every extreme that they name: `routing`: among the 64 sequences of one index of ep, no expert is chosen more than 16 times, and some expert is chosen exactly 16 times; a sequence's 2 choices differ.
All inputs are finite; a program needn't handle non-finite values.
Results may differ from the reference program's by a relative error of at most 0.017.
Values may be sent and summed in bfloat16 or wider, within the bound.
A program may use at most 192 MiB of HBM per device.

```python
import math
import jax
import jax.numpy as jnp
import numpy as np
from jax import lax

D = 2048
HEADS = 16
HEAD = 64
LOW = 64
DFF = 5632
EFF = 1536
TOPK = 2
SEQS = 64
SEQUENCES = 1024
EXPERTS = 16
CAP = 16
N_EP = 16
N_TP = 2


def block_scale(stream_key, dims, pieces, least, largest):
    def one(position, blocks):
        steps = jax.random.uniform(jax.random.fold_in(jax.random.fold_in(stream_key, 6), position), (blocks,), jnp.float32, least / len(pieces), largest / len(pieces))
        return jnp.repeat(jnp.exp(steps), dims[position] // blocks).reshape((-1,) + (1,) * (len(dims) - position - 1))

    factor_of = one(*pieces[0])
    for cut in pieces[1:]:
        factor_of = factor_of * one(*cut)
    return factor_of


def assign_block(own_key, own, number, rows, number_of, top, most, lean):
    ranking = jax.random.permutation(own_key, number_of)
    packed, common = portions_of(number_of, rows * top, most, lean, True), portions_of(number_of, rows * top, most, lean, False)
    places = jnp.arange(number_of)

    def named(sizes, offset_by):
        used = int((sizes > 0).sum())
        fixed = max(1, used // 4)
        passed = fixed + (places - fixed + offset_by * (used - fixed)) % max(1, number_of - fixed)
        return jnp.zeros((number_of,), jnp.int32).at[ranking[jnp.where(places < fixed, places, passed)]].set(jnp.asarray(sizes, jnp.int32))

    sizes = jnp.where(number % 4 == 0, named(packed, number // 4), named(common, number - number // 4 - 1))
    mixed = jax.random.permutation(jax.random.fold_in(own, 3), number_of)
    donor, receiver = mixed[0:number_of // 2 * 2:2], mixed[1:number_of // 2 * 2:2]
    slack = jnp.minimum(sizes[donor] - 1, most - sizes[receiver]) // 2
    slack = jnp.where((donor == ranking[0]) | (receiver == ranking[0]) | (sizes[receiver] == 0), 0, jnp.maximum(slack, 0))
    passed = jax.random.randint(jax.random.fold_in(own, 4), (number_of // 2,), 0, 1 << 20) % (slack + 1)
    sizes = sizes.at[donor].add(-passed).at[receiver].add(passed)
    members = jnp.searchsorted(jnp.cumsum(sizes), jnp.arange(rows * top), side="right").astype(jnp.int32)
    listing = members.reshape(top, rows).T
    listing = listing[jax.random.permutation(jax.random.fold_in(own, 1), rows)]
    offset_by = jax.random.randint(jax.random.fold_in(own, 2), (rows, 1), 0, top)
    return jnp.take_along_axis(listing, (jnp.arange(top)[None, :] + offset_by) % top, axis=1)


def portions_of(count, total, most, lean, full):
    portions = [(1 << 20) // math.isqrt(grade ** lean) + 1 for grade in range(1, count + 1)]
    largest = most if full else min(most, max(-(-total // count), total * portions[0] // sum(portions)))
    least = 1 if total - largest >= count - 1 else 0
    counts, rest = [largest] + [least] * (count - 1), total - largest - least * (count - 1)
    while rest > 0:
        movable = [i for i in range(1, count) if counts[i] < largest] or [i for i in range(1, count) if counts[i] < most]
        pool, remaining = sum([portions[i] for i in movable]), rest
        for i in movable:
            extra = min(most - counts[i], max(1, remaining * portions[i] // pool), rest)
            counts[i] = counts[i] + extra
            rest = rest - extra
    return np.array(counts)


def scatter_about(key, shape, width, bound, pieces=(), held_as=jnp.bfloat16):
    values = jax.random.normal(key, shape, jnp.float32) * width
    if len(pieces) > 0:
        values = block_scale(key, shape, pieces, -0.22, 0.18) * values
    return jnp.clip(values, min=-bound, max=bound).astype(held_as)


def setup_inputs(seed: int = 0) -> dict:
    arg_keys = jax.random.split(jax.random.key(seed), 25)
    hidden = scatter_about(arg_keys[0], (SEQUENCES, D), 1.0, 6.0, ((0, 16),))
    mix_gain = jnp.clip(1.0 + 0.18 * jax.random.normal(arg_keys[1], (D,), jnp.float32), 0.1, 1.9)
    recept_weight = scatter_about(arg_keys[2], (D, HEADS * HEAD), D ** -0.5, 0.125, ((1, 2),))
    key_weight = scatter_about(arg_keys[3], (D, HEADS * HEAD), D ** -0.5, 0.125, ((1, 2),))
    value_weight = scatter_about(arg_keys[4], (D, HEADS * HEAD), D ** -0.5, 0.125, ((1, 2),))
    decay_down = scatter_about(arg_keys[5], (D, LOW), D ** -0.5, 0.125)
    decay_up = scatter_about(arg_keys[6], (LOW, HEADS * HEAD), LOW ** -0.5, 0.75)
    decay_bias = jnp.clip(jax.random.uniform(arg_keys[7], (HEADS * HEAD,), jnp.float32, -4.0, 1.0), -4.0, 1.0)
    rate_down = scatter_about(arg_keys[8], (D, LOW), D ** -0.5, 0.125)
    rate_up = scatter_about(arg_keys[9], (LOW, HEADS * HEAD), LOW ** -0.5, 0.75)
    rate_bias = scatter_about(arg_keys[10], (HEADS * HEAD,), 1.0, 4.0, (), jnp.float32)
    head_gain = jnp.clip(1.0 + 0.18 * jax.random.normal(arg_keys[11], (HEADS * HEAD,), jnp.float32), 0.1, 1.9)
    out_weight = scatter_about(arg_keys[12], (HEADS * HEAD, D), (HEADS * HEAD) ** -0.5, 0.1875, ((0, 2),))
    memory_state = scatter_about(arg_keys[13], (SEQUENCES, HEADS, HEAD, HEAD), 1.0, 6.0, ((0, 16), (1, 2)), jnp.float32)
    ffn_gain = jnp.clip(1.0 + 0.18 * jax.random.normal(arg_keys[14], (D,), jnp.float32), 0.1, 1.9)
    blend_vector = scatter_about(arg_keys[15], (D,), D ** -0.5, 0.125)
    dense_gate = scatter_about(arg_keys[16], (D, DFF), D ** -0.5, 0.125, ((1, 32),))
    dense_up = scatter_about(arg_keys[17], (D, DFF), D ** -0.5, 0.125, ((1, 32),))
    dense_down = scatter_about(arg_keys[18], (DFF, D), (DFF // 16) ** -0.5, 0.3125, ((0, 32),))
    expert_gate = scatter_about(arg_keys[19], (EXPERTS, D, EFF), D ** -0.5, 0.125, ((0, 16), (2, 2)))
    expert_up = scatter_about(arg_keys[20], (EXPERTS, D, EFF), D ** -0.5, 0.125, ((0, 16), (2, 2)))
    expert_down = scatter_about(arg_keys[21], (EXPERTS, EFF, D), EFF ** -0.5, 0.15625, ((0, 16), (1, 2)))
    routing_keys = jax.random.split(jax.random.fold_in(arg_keys[22], 1), SEQUENCES // SEQS)
    routing_turns = jax.random.permutation(jax.random.fold_in(arg_keys[22], 3), SEQUENCES // SEQS)
    routing = jax.vmap(lambda own, number: assign_block(jax.random.fold_in(arg_keys[22], 2), own, number, SEQS, EXPERTS, TOPK, CAP, 1))(routing_keys, routing_turns).reshape((SEQUENCES, TOPK))
    route_scale = jnp.clip(0.25 + 0.75 * jax.random.uniform(arg_keys[23], (SEQUENCES, TOPK), jnp.float32) ** block_scale(arg_keys[23], (SEQUENCES, TOPK), ((0, 16),), -0.2, 0.2), 0.25, 1.0)
    return {"hidden": hidden, "mix_gain": mix_gain, "recept_weight": recept_weight, "key_weight": key_weight, "value_weight": value_weight, "decay_down": decay_down, "decay_up": decay_up, "decay_bias": decay_bias, "rate_down": rate_down, "rate_up": rate_up, "rate_bias": rate_bias, "head_gain": head_gain, "out_weight": out_weight, "memory_state": memory_state, "ffn_gain": ffn_gain, "blend_vector": blend_vector, "dense_gate": dense_gate, "dense_up": dense_up, "dense_down": dense_down, "expert_gate": expert_gate, "expert_up": expert_up, "expert_down": expert_down, "routing": routing, "route_scale": route_scale}


def stored(tensor):
    return lax.optimization_barrier(tensor.astype(jnp.bfloat16)).astype(jnp.float32)

def rms_scaled(tensor, gain_vec):
    values = tensor.astype(jnp.float32)
    return values * lax.rsqrt(lax.optimization_barrier(jnp.mean(values * values, axis=-1, keepdims=True)) + 1e-06) * gain_vec

def silu_of(tensor):
    return tensor / (1.0 + jnp.exp(-tensor))

def matmul(left, right):
    return jnp.dot(left, right, preferred_element_type=jnp.float32)

def reference(hidden, mix_gain, recept_weight, key_weight, value_weight, decay_down, decay_up, decay_bias, rate_down, rate_up, rate_bias, head_gain, out_weight, memory_state, ffn_gain, blend_vector, dense_gate, dense_up, dense_down, expert_gate, expert_up, expert_down, routing, route_scale):
    seq_count = hidden.shape[0]
    full_width = HEADS * HEAD
    normed_in = rms_scaled(hidden, mix_gain).astype(jnp.bfloat16)
    recept_rows = stored(matmul(normed_in, recept_weight)).reshape(seq_count, HEADS, HEAD)
    key_rows = stored(matmul(normed_in, key_weight)).reshape(seq_count, HEADS, HEAD)
    value_rows = stored(matmul(normed_in, value_weight)).reshape(seq_count, HEADS, HEAD)
    decay_low = jnp.tanh(matmul(normed_in, decay_down)).astype(jnp.bfloat16)
    decay_pre = matmul(decay_low, decay_up) + decay_bias
    decay_rate = jnp.exp(-jnp.exp(-jax.nn.softplus(-decay_pre) - 0.5)).reshape(seq_count, HEADS, HEAD)
    rate_low = matmul(normed_in, rate_down).astype(jnp.bfloat16)
    learn_rate = jax.nn.sigmoid(matmul(rate_low, rate_up) + rate_bias).reshape(seq_count, HEADS, HEAD)
    unit_key = key_rows * lax.rsqrt(lax.optimization_barrier(jnp.sum(key_rows * key_rows, axis=-1, keepdims=True)) + 1e-06)
    removed = jnp.einsum('shij,shj->shi', memory_state, unit_key, precision=lax.Precision.HIGHEST)
    new_state = memory_state * decay_rate[:, :, None, :] - removed[..., None] * (unit_key * learn_rate)[:, :, None, :] + value_rows[..., None] * (key_rows * learn_rate)[:, :, None, :]
    readout = jnp.einsum('shij,shj->shi', new_state, recept_rows, precision=lax.Precision.HIGHEST)
    centre = lax.optimization_barrier(jnp.mean(readout, axis=-1, keepdims=True))
    variance = lax.optimization_barrier(jnp.mean(jnp.square(readout - centre), axis=-1, keepdims=True))
    head_normed = ((readout - centre) * lax.rsqrt(variance + 0.00064) * head_gain.reshape(HEADS, HEAD)).astype(jnp.bfloat16).reshape(seq_count, full_width)
    group_width = full_width // N_TP
    attn_sum = jnp.zeros((seq_count, D), jnp.float32)
    for group in range(N_TP):
        lower = group * group_width
        attn_sum = attn_sum + stored(matmul(head_normed[:, lower:lower + group_width], out_weight[lower:lower + group_width]))
    first_res = (hidden.astype(jnp.float32) + attn_sum).astype(jnp.bfloat16)
    ffn_in = rms_scaled(first_res, ffn_gain).astype(jnp.bfloat16)
    blend = jax.nn.sigmoid(jnp.dot(ffn_in, blend_vector, preferred_element_type=jnp.float32))
    dense_act = (silu_of(matmul(ffn_in, dense_gate)) * matmul(ffn_in, dense_up)).astype(jnp.bfloat16)
    dense_out = matmul(dense_act, dense_down)
    flat_route = routing.reshape(-1)
    flat_scale = route_scale.reshape(-1)
    slot_total = N_EP * CAP
    slot_index = jnp.arange(slot_total, dtype=jnp.int32)

    def one_expert(total, inputs):
        gate_mat, up_mat, down_mat, index = inputs
        chosen = flat_route == index
        live_count = jnp.sum(chosen.astype(jnp.int32))
        picks = jnp.nonzero(chosen, size=slot_total, fill_value=0)[0].astype(jnp.int32)
        owners = (picks // TOPK).astype(jnp.int32)
        rows = ffn_in[owners]
        live = slot_index < live_count
        scales = jnp.where(live, flat_scale[picks], jnp.zeros_like(flat_scale[picks]))
        expert_act = (silu_of(matmul(rows, gate_mat)) * matmul(rows, up_mat)).astype(jnp.bfloat16)
        expert_out = matmul(expert_act, down_mat)
        return (total.at[owners].add(expert_out * scales[:, None]), None)
    expert_sum, _ = lax.scan(one_expert, jnp.zeros((seq_count, D), jnp.float32), (expert_gate, expert_up, expert_down, jnp.arange(EXPERTS, dtype=jnp.int32)))
    layer_out = (first_res.astype(jnp.float32) + expert_sum + blend[:, None] * dense_out).astype(jnp.bfloat16)
    return (layer_out, new_state)
```

```python
import functools
import math

import jax
import jax.numpy as jnp
from jax import lax
from jax.experimental import pallas as pl
from jax.experimental.pallas import tpu as pltpu
from jax.sharding import PartitionSpec as P

MESH = pl.DeviceIdType.MESH
F32 = jnp.float32
BF16 = jnp.bfloat16
VMEM_LIMIT = 64 * 1024 * 1024 - 65536
VMEM_SPEC = pl.BlockSpec(memory_space=pltpu.VMEM)


def matmul(left, right):
    return jnp.dot(left, right, preferred_element_type=F32)


def silu_of(tensor):
    return tensor / (1.0 + jnp.exp(-tensor))


def rms_scaled(values, gain):
    return values * lax.rsqrt(jnp.mean(values * values, axis=-1, keepdims=True) + 1e-06) * gain


def factors_of(count):
    slow = 4 if count % 4 == 0 else 1
    rest = count // slow
    mid = math.isqrt(rest)
    while rest % mid:
        mid -= 1
    return slow, mid, rest // mid


def attention_kernel(
    step_rows,
    hidden,
    mix_gain,
    recept_weight,
    key_weight,
    value_weight,
    decay_down,
    decay_up,
    decay_bias,
    rate_down,
    rate_up,
    rate_bias,
    head_gain,
    out_weight,
    state_in,
    state_out,
    partial,
    recept_s,
    unit_s,
    unit_rate_s,
    key_rate_s,
    value_s,
    decay_s,
    readout_s,
    normed_s,
):
    step = pl.program_id(0)
    heads, seqs, size = recept_s.shape
    width = heads * size
    own = pl.ds(pl.multiple_of(lax.axis_index("tp") * width, 128), width)

    @pl.when(step == 0)
    def _():
        normed = rms_scaled(hidden[...].astype(F32), mix_gain[...]).astype(BF16)
        recept = matmul(normed, recept_weight[...]).astype(BF16).astype(F32)
        keys = matmul(normed, key_weight[...]).astype(BF16).astype(F32)
        vals = matmul(normed, value_weight[...]).astype(BF16).astype(F32)
        decay_low = jnp.tanh(matmul(normed, decay_down[...])).astype(BF16)
        decay_pre = matmul(decay_low, decay_up[:, own]) + decay_bias[:, own]
        softplus = jnp.maximum(-decay_pre, 0.0) + jnp.log1p(jnp.exp(-jnp.abs(decay_pre)))
        decay = jnp.exp(-jnp.exp(-softplus - 0.5))
        rate_low = matmul(normed, rate_down[...]).astype(BF16)
        rate = 1.0 / (1.0 + jnp.exp(-(matmul(rate_low, rate_up[:, own]) + rate_bias[:, own])))
        for h in range(heads):
            cols = slice(h * size, (h + 1) * size)
            key_h, rate_h = keys[:, cols], rate[:, cols]
            unit = key_h * lax.rsqrt(jnp.sum(key_h * key_h, axis=-1, keepdims=True) + 1e-06)
            recept_s[h] = recept[:, cols]
            unit_s[h] = unit
            unit_rate_s[h] = unit * rate_h
            key_rate_s[h] = key_h * rate_h
            value_s[h] = vals[:, cols]
            decay_s[h] = decay[:, cols]

    eye = (
        lax.broadcasted_iota(jnp.int32, (size, size), 0)
        == lax.broadcasted_iota(jnp.int32, (size, size), 1)
    ).astype(F32)

    def one_sequence(local, carry):
        row = pl.ds(step * step_rows + local, 1)
        for h in range(heads):
            state = state_in[local, h]
            removed = jnp.sum(state * unit_s[h, row], axis=-1, keepdims=True)
            value = jnp.sum(eye * value_s[h, row], axis=-1, keepdims=True)
            new = (
                state * decay_s[h, row]
                - removed * unit_rate_s[h, row]
                + value * key_rate_s[h, row]
            )
            state_out[local, h] = new
            out = jnp.sum(new * recept_s[h, row], axis=-1, keepdims=True)
            readout_s[h, row] = jnp.sum(eye * out, axis=0, keepdims=True)
        return carry

    lax.fori_loop(0, step_rows, one_sequence, 0)

    @pl.when(step == pl.num_programs(0) - 1)
    def _():
        gain = head_gain[:, own]
        for h in range(heads):
            cols = slice(h * size, (h + 1) * size)
            out = readout_s[h]
            centred = out - jnp.mean(out, axis=-1, keepdims=True)
            variance = jnp.mean(centred * centred, axis=-1, keepdims=True)
            normed_s[:, cols] = (centred * lax.rsqrt(variance + 0.00064) * gain[:, cols]).astype(BF16)
        partial[...] = matmul(normed_s[...], out_weight[...]).astype(BF16)


def attention(hidden, vectors, state):
    seqs, heads, size, _ = state.shape
    width = heads * size
    step_rows = math.gcd(seqs, 8)
    block = pl.BlockSpec((step_rows, heads, size, size), lambda i: (i, 0, 0, 0))
    operands = (hidden,) + vectors
    whole = [pl.BlockSpec(a.shape, lambda i: (0, 0)) for a in operands]
    per_head = pltpu.VMEM((heads, seqs, size), F32)
    return pl.pallas_call(
        functools.partial(attention_kernel, step_rows),
        grid=(seqs // step_rows,),
        out_shape=(
            jax.ShapeDtypeStruct(state.shape, F32),
            jax.ShapeDtypeStruct(hidden.shape, BF16),
        ),
        in_specs=whole + [block],
        out_specs=(block, pl.BlockSpec(hidden.shape, lambda i: (0, 0))),
        scratch_shapes=[per_head] * 7 + [pltpu.VMEM((seqs, width), BF16)],
        compiler_params=pltpu.CompilerParams(
            dimension_semantics=("arbitrary",), vmem_limit_bytes=VMEM_LIMIT
        ),
        name="attention",
    )(*operands, state)


def position(sizes):
    ep = lax.axis_index("ep")
    strides = (sizes[1] * sizes[2], sizes[2], 1)
    return ep, tuple(ep // s % n for s, n in zip(strides, sizes)), strides


def greet_all(count):
    ep, tp = lax.axis_index("ep"), lax.axis_index("tp")
    barrier = pltpu.get_barrier_semaphore()

    def greet(k, carry):
        pl.semaphore_signal(
            barrier, inc=1, device_id=((ep + k) % count, tp), device_id_type=MESH
        )
        return carry

    lax.fori_loop(1, count, greet, 0)
    pl.semaphore_signal(barrier, inc=1, device_id=(ep, 1 - tp), device_id_type=MESH)
    pl.semaphore_wait(barrier, count)


def remote(src, dst, send, recv, device):
    return pltpu.make_async_remote_copy(
        src_ref=src,
        dst_ref=dst,
        send_sem=send,
        recv_sem=recv,
        device_id=device,
        device_id_type=MESH,
    )


def gather_kernel(
    sizes,
    partial,
    hidden,
    gain,
    meta,
    first,
    tokens,
    metas,
    sibling_part,
    part_sem,
    meta_send,
    meta_recv,
    own_sem,
    send_sem,
    recv_sem,
    pass_send,
    pass_recv,
):
    count = sizes[0] * sizes[1] * sizes[2]
    ep, at, strides = position(sizes)
    tp = lax.axis_index("tp")
    half = first.shape[0]
    mine = pl.ds(pl.multiple_of(tp * half, half), half)
    other = pl.ds(pl.multiple_of((1 - tp) * half, half), half)
    greet_all(count)
    swap = remote(partial.at[other], sibling_part, part_sem.at[0], part_sem.at[1], (ep, 1 - tp))
    swap.start()

    def meta_copy(k):
        return remote(
            meta, metas.at[ep], meta_send.at[k], meta_recv.at[k], ((ep + k) % count, tp)
        )

    def start_meta(k, carry):
        meta_copy(k).start()
        return carry

    lax.fori_loop(1, count, start_meta, 0)
    metas[ep] = meta[...]
    swap.wait()
    total = (
        hidden[mine, :].astype(F32)
        + partial[mine, :].astype(F32)
        + sibling_part[...].astype(F32)
    ).astype(BF16)
    first[...] = total
    ffn_in = rms_scaled(total.astype(F32), gain[...]).astype(BF16)
    tokens[at[0], at[1], at[2], mine, :] = ffn_in

    def blocks(order):
        held = [pl.ds(c, 1) for c in at]
        for d in order:
            before = tuple(held)
            for k in range(1, sizes[d]):
                come = list(held)
                come[d] = pl.ds((at[d] + sizes[d] - k) % sizes[d], 1)
                yield d, k, before, tuple(come)
            held[d] = pl.ds(0, sizes[d])

    def run(core, order, order_of_other):
        rows = pl.ds(core * half, half)
        rows_of_other = pl.ds((1 - core) * half, half)
        sibling = (ep, 1 - core)

        def own_copy(r):
            view = tokens.at[pl.ds(at[0], 1), pl.ds(at[1], 1), pl.ds(at[2], 1), r]
            return remote(view, view, own_sem.at[0], own_sem.at[1], sibling)

        def pass_copy(d, k, come, r):
            view = tokens.at[come + (r,)]
            return remote(view, view, pass_send.at[d, k], pass_recv.at[d, k], sibling)

        to_wait = [own_copy(rows)]
        to_wait[0].start()
        steps = list(blocks(order))
        for d in order:
            copies = []
            for dd, k, before, come in steps:
                if dd == d:
                    peer = ep + ((at[d] + k) % sizes[d] - at[d]) * strides[d]
                    view = tokens.at[before + (rows,)]
                    copy = remote(view, view, send_sem.at[d, k], recv_sem.at[d, k], (peer, core))
                    copy.start()
                    copies.append((copy, k, come))
            for copy, k, come in copies:
                copy.wait()
                onward = pass_copy(d, k, come, rows)
                onward.start()
                to_wait.append(onward)
        for copy in to_wait:
            copy.wait_send()
        own_copy(rows_of_other).wait_recv()
        for d, k, before, come in blocks(order_of_other):
            pass_copy(d, k, come, rows_of_other).wait_recv()

    @pl.when(tp == 0)
    def _():
        run(0, (2, 1, 0), (0, 1, 2))

    @pl.when(tp == 1)
    def _():
        run(1, (0, 1, 2), (2, 1, 0))

    def wait_meta(k, carry):
        meta_copy(k).wait()
        return carry

    lax.fori_loop(1, count, wait_meta, 0)


def gather_tokens(sizes, partial, hidden, gain, meta):
    seqs, width = hidden.shape
    count = sizes[0] * sizes[1] * sizes[2]
    half = seqs // 2
    most = max(sizes)
    dma = pltpu.SemaphoreType.DMA
    return pl.pallas_call(
        functools.partial(gather_kernel, sizes),
        out_shape=(
            jax.ShapeDtypeStruct((half, width), BF16),
            jax.ShapeDtypeStruct(sizes + (seqs, width), BF16),
            jax.ShapeDtypeStruct((count,) + meta.shape, F32),
        ),
        in_specs=[VMEM_SPEC] * 4,
        out_specs=(VMEM_SPEC,) * 3,
        scratch_shapes=[
            pltpu.VMEM((half, width), BF16),
            dma((2,)),
            dma((count,)),
            dma((count,)),
            dma((2,)),
            dma((3, most)),
            dma((3, most)),
            dma((3, most)),
            dma((3, most)),
        ],
        compiler_params=pltpu.CompilerParams(
            collective_id=0, has_side_effects=True, vmem_limit_bytes=VMEM_LIMIT
        ),
        name="gather_tokens",
    )(partial, hidden, gain, meta)


def scatter_kernel(sizes, parts, first, out, total, from_sibling, land0, land1, sems):
    pair_send, pair_recv, send_sem, recv_sem, last_sem = sems
    ep, at, strides = position(sizes)
    tp = lax.axis_index("tp")
    half = first.shape[0]
    mine = pl.ds(pl.multiple_of(tp * half, half), half)
    other = pl.ds(pl.multiple_of((1 - tp) * half, half), half)
    greet_all(sizes[0] * sizes[1] * sizes[2])
    pairs = []
    for z in range(sizes[0]):
        copy = remote(
            parts.at[z, :, :, other],
            from_sibling.at[z],
            pair_send.at[z],
            pair_recv.at[z],
            (ep, 1 - tp),
        )
        copy.start()
        pairs.append(copy)
    per = sizes[1] * sizes[2]
    for z in range(sizes[0]):
        pairs[z].wait()

        def add(b, carry, z=z):
            y, x = b // sizes[2], b % sizes[2]
            total[z, y, x] = (
                parts[z, y, x, mine, :].astype(F32) + from_sibling[z, y, x].astype(F32)
            ).astype(BF16)
            return carry

        lax.fori_loop(0, per, add, 0)

    def run(core, order, lands):
        held = [pl.ds(0, n) for n in sizes]
        for place, d in enumerate(order):
            land = lands[place]
            copies = []
            for k in range(1, sizes[d]):
                goal = (at[d] + k) % sizes[d]
                view = list(held)
                view[d] = pl.ds(goal, 1)
                copy = remote(
                    total.at[tuple(view)],
                    land.at[k - 1],
                    send_sem.at[d, k],
                    recv_sem.at[d, k],
                    (ep + (goal - at[d]) * strides[d], core),
                )
                copy.start()
                copies.append(copy)
            for copy in copies:
                copy.wait()
            held[d] = pl.ds(at[d], 1)
            box = [land.shape[1 + i] for i in range(3)]
            last = place == len(order) - 1
            flat = box[0] * box[1] * box[2]

            def gather_sum(b, carry, land=land, box=box, last=last, fixed=tuple(held)):
                inner = (b // (box[1] * box[2]), b // box[2] % box[1], b % box[2])
                spot = tuple(at[i] if box[i] == 1 else inner[i] for i in range(3))
                value = total[spot].astype(F32)
                for k in range(land.shape[0]):
                    value = value + land[(k,) + inner].astype(F32)
                if last:
                    out[pl.ds(core * half, half), :] = (first[...].astype(F32) + value).astype(BF16)
                else:
                    total[spot] = value.astype(BF16)
                return carry

            lax.fori_loop(0, flat, gather_sum, 0)

    @pl.when(tp == 0)
    def _():
        run(0, (0, 1, 2), land0)

    @pl.when(tp == 1)
    def _():
        run(1, (2, 1, 0), land1)

    swap = remote(out.at[mine], out.at[mine], last_sem.at[0], last_sem.at[1], (ep, 1 - tp))
    swap.start()
    swap.wait()


def landing(sizes, order, half, width):
    box = list(sizes)
    shapes = []
    for d in order:
        box[d] = 1
        shapes.append(pltpu.VMEM((max(1, sizes[d] - 1),) + tuple(box) + (half, width), BF16))
    return shapes


def scatter_sum(sizes, parts, first):
    half, width = first.shape
    most = max(sizes)
    dma = pltpu.SemaphoreType.DMA
    return pl.pallas_call(
        functools.partial(scatter_kernel, sizes),
        out_shape=jax.ShapeDtypeStruct((2 * half, width), BF16),
        in_specs=[VMEM_SPEC] * 2,
        out_specs=VMEM_SPEC,
        scratch_shapes=[
            pltpu.VMEM(sizes + (half, width), BF16),
            pltpu.VMEM(sizes + (half, width), BF16),
            landing(sizes, (0, 1, 2), half, width),
            landing(sizes, (2, 1, 0), half, width),
            [dma((sizes[0],)), dma((sizes[0],)), dma((3, most)), dma((3, most)), dma((2,))],
        ],
        compiler_params=pltpu.CompilerParams(
            collective_id=1, has_side_effects=True, vmem_limit_bytes=VMEM_LIMIT
        ),
        name="scatter_sum",
    )(parts, first)


def shards(
    hidden,
    mix_gain,
    recept_weight,
    key_weight,
    value_weight,
    decay_down,
    decay_up,
    decay_bias,
    rate_down,
    rate_up,
    rate_bias,
    head_gain,
    out_weight,
    memory_state,
    ffn_gain,
    blend_vector,
    dense_gate,
    dense_up,
    dense_down,
    expert_gate,
    expert_up,
    expert_down,
    routing,
    route_scale,
):
    seqs, width = hidden.shape
    count = lax.axis_size("ep")
    sizes = factors_of(count)
    top = routing.shape[1]
    cap = max(2, 2 * seqs * top // count)
    new_state, partial = attention(
        hidden,
        (
            mix_gain[None],
            recept_weight,
            key_weight,
            value_weight,
            decay_down,
            decay_up,
            decay_bias[None],
            rate_down,
            rate_up,
            rate_bias[None],
            head_gain[None],
            out_weight,
        ),
        memory_state,
    )
    meta = jnp.concatenate([routing.T.astype(F32), route_scale.T], axis=0)
    meta = jnp.pad(meta, ((0, -2 * top % 8), (0, -seqs % 128)))
    first, tokens, metas = gather_tokens(sizes, partial, hidden, ffn_gain[None], meta)
    tokens = tokens.reshape(count * seqs, width)

    hit = metas[:, :top, :seqs] == lax.axis_index("ep").astype(F32)
    chosen = jnp.any(hit, axis=1)
    scale_of = jnp.sum(jnp.where(hit, metas[:, top : 2 * top, :seqs], 0.0), axis=1)
    earlier = jnp.arange(seqs)[:, None] < jnp.arange(seqs)[None, :]
    rank = matmul(chosen.astype(BF16), earlier.astype(BF16)).astype(jnp.int32)
    place = jnp.where(chosen, rank + jnp.arange(count, dtype=jnp.int32)[:, None] * cap, -1)
    select = place.reshape(1, -1) == jnp.arange(count * cap, dtype=jnp.int32)[:, None]
    slot_scale = jnp.sum(jnp.where(select, scale_of.reshape(1, -1), 0.0), axis=1, keepdims=True)
    picked = matmul(select.astype(BF16), tokens).astype(BF16)
    expert_act = (silu_of(matmul(picked, expert_gate[0])) * matmul(picked, expert_up[0])).astype(BF16)
    expert_out = (matmul(expert_act, expert_down[0]) * slot_scale).astype(BF16)
    blend = jax.nn.sigmoid(matmul(tokens, blend_vector[:, None]))
    dense_act = (
        silu_of(matmul(tokens, dense_gate)) * matmul(tokens, dense_up) * blend
    ).astype(BF16)
    spread = (place.reshape(-1, 1) == jnp.arange(count * cap, dtype=jnp.int32)[None, :]).astype(BF16)
    parts = matmul(
        jnp.concatenate([spread, dense_act], axis=1),
        jnp.concatenate([expert_out, dense_down], axis=0),
    ).astype(BF16)
    layer_out = scatter_sum(sizes, parts.reshape(sizes + (seqs, width)), first)
    return (layer_out, new_state)


def solution(mesh):
    in_specs = (
        P("ep", None),
        P(),
        P(None, "tp"),
        P(None, "tp"),
        P(None, "tp"),
        P(),
        P(),
        P(),
        P(),
        P(),
        P(),
        P(),
        P("tp", None),
        P("ep", "tp", None, None),
        P(),
        P(),
        P(None, ("ep", "tp")),
        P(None, ("ep", "tp")),
        P(("ep", "tp"), None),
        P("ep", None, "tp"),
        P("ep", None, "tp"),
        P("ep", "tp", None),
        P("ep", None),
        P("ep", None),
    )
    out_specs = (P("ep", None), P("ep", "tp", None, None))
    return jax.shard_map(shards, mesh=mesh, in_specs=in_specs, out_specs=out_specs, check_vma=False)
```

```python
import functools
import math

import jax
import jax.numpy as jnp
from jax import lax
from jax.experimental import pallas as pl
from jax.experimental.pallas import tpu as pltpu
from jax.sharding import PartitionSpec as P

MESH = pl.DeviceIdType.MESH
F32 = jnp.float32
BF16 = jnp.bfloat16
VMEM_LIMIT = 64 * 1024 * 1024 - 65536
VMEM_SPEC = pl.BlockSpec(memory_space=pltpu.VMEM)


def matmul(left, right):
    return jnp.dot(left, right, preferred_element_type=F32)


def matmul_nt(left, right):
    return lax.dot_general(left, right, (((1,), (1,)), ((), ())), preferred_element_type=F32)


def silu_of(tensor):
    return tensor / (1.0 + jnp.exp(-tensor))


def rms_scaled(values, gain):
    return values * lax.rsqrt(jnp.mean(values * values, axis=-1, keepdims=True) + 1e-06) * gain


def factors_of(count):
    slow = 4 if count % 4 == 0 else 1
    rest = count // slow
    mid = math.isqrt(rest)
    while rest % mid:
        mid -= 1
    return slow, mid, rest // mid


def attention_kernel(
    step_rows,
    hidden,
    mix_gain,
    recept_weight,
    key_weight,
    value_weight,
    decay_down,
    decay_up,
    decay_bias,
    rate_down,
    rate_up,
    rate_bias,
    head_gain,
    out_weight,
    state_in,
    state_out,
    partial,
    recept_s,
    unit_s,
    unit_rate_s,
    key_rate_s,
    value_s,
    decay_s,
    readout_s,
    normed_s,
):
    step = pl.program_id(0)
    heads, seqs, size = recept_s.shape
    width = heads * size
    own = pl.ds(pl.multiple_of(lax.axis_index("tp") * width, 128), width)

    @pl.when(step == 0)
    def _():
        normed = rms_scaled(hidden[...].astype(F32), mix_gain[...]).astype(BF16)
        recept = matmul(normed, recept_weight[...]).astype(BF16).astype(F32)
        keys = matmul(normed, key_weight[...]).astype(BF16).astype(F32)
        vals = matmul(normed, value_weight[...]).astype(BF16).astype(F32)
        decay_low = jnp.tanh(matmul_nt(normed, decay_down[...])).astype(BF16)
        decay_pre = matmul(decay_low, decay_up[:, own]) + decay_bias[:, own]
        softplus = jnp.maximum(-decay_pre, 0.0) + jnp.log1p(jnp.exp(-jnp.abs(decay_pre)))
        decay = jnp.exp(-jnp.exp(-softplus - 0.5))
        rate_low = matmul_nt(normed, rate_down[...]).astype(BF16)
        rate = 1.0 / (1.0 + jnp.exp(-(matmul(rate_low, rate_up[:, own]) + rate_bias[:, own])))
        for h in range(heads):
            cols = slice(h * size, (h + 1) * size)
            key_h, rate_h = keys[:, cols], rate[:, cols]
            unit = key_h * lax.rsqrt(jnp.sum(key_h * key_h, axis=-1, keepdims=True) + 1e-06)
            recept_s[h] = recept[:, cols]
            unit_s[h] = unit
            unit_rate_s[h] = unit * rate_h
            key_rate_s[h] = key_h * rate_h
            value_s[h] = vals[:, cols]
            decay_s[h] = decay[:, cols]

    tall = (16, size)
    place = lax.broadcasted_iota(jnp.int32, tall, 0)

    def wide(row):
        return jnp.broadcast_to(row, tall)

    def one_sequence(local, carry):
        row = pl.ds(step * step_rows + local, 1)
        for h in range(heads):
            state = state_in[local, h]
            removed = matmul_nt(wide(unit_s[h, row]).astype(BF16), state.astype(BF16))
            left = jnp.where(place == 0, -removed, wide(value_s[h, row])).astype(BF16)
            key_rate = wide(key_rate_s[h, row])
            rest = key_rate - key_rate.astype(BF16).astype(F32)
            right = jnp.where(
                place == 0,
                wide(unit_rate_s[h, row]),
                jnp.where(place == 1, key_rate, jnp.where(place == 2, rest, 0.0)),
            ).astype(BF16)
            new = state * decay_s[h, row] + lax.dot_general(
                left, right, (((0,), (0,)), ((), ())), preferred_element_type=F32
            )
            state_out[local, h] = new
            out = matmul_nt(wide(recept_s[h, row]).astype(BF16), new.astype(BF16))
            readout_s[h, row] = out[0:1]
        return carry

    lax.fori_loop(0, step_rows, one_sequence, 0)

    @pl.when(step == pl.num_programs(0) - 1)
    def _():
        gain = head_gain[:, own]
        for h in range(heads):
            cols = slice(h * size, (h + 1) * size)
            out = readout_s[h]
            centred = out - jnp.mean(out, axis=-1, keepdims=True)
            variance = jnp.mean(centred * centred, axis=-1, keepdims=True)
            normed_s[:, cols] = (centred * lax.rsqrt(variance + 0.00064) * gain[:, cols]).astype(BF16)
        partial[...] = matmul(normed_s[...], out_weight[...]).astype(BF16)


def attention(hidden, vectors, state):
    seqs, heads, size, _ = state.shape
    width = heads * size
    step_rows = math.gcd(seqs, 8)
    block = pl.BlockSpec((step_rows, heads, size, size), lambda i: (i, 0, 0, 0))
    operands = (hidden,) + vectors
    whole = [pl.BlockSpec(a.shape, lambda i: (0, 0)) for a in operands]
    per_head = pltpu.VMEM((heads, seqs, size), F32)
    return pl.pallas_call(
        functools.partial(attention_kernel, step_rows),
        grid=(seqs // step_rows,),
        out_shape=(
            jax.ShapeDtypeStruct(state.shape, F32),
            jax.ShapeDtypeStruct(hidden.shape, BF16),
        ),
        in_specs=whole + [block],
        out_specs=(block, pl.BlockSpec(hidden.shape, lambda i: (0, 0))),
        scratch_shapes=[per_head] * 7 + [pltpu.VMEM((seqs, width), BF16)],
        compiler_params=pltpu.CompilerParams(
            dimension_semantics=("arbitrary",), vmem_limit_bytes=VMEM_LIMIT
        ),
        name="attention",
    )(*operands, state)


def position(sizes):
    ep = lax.axis_index("ep")
    strides = (sizes[1] * sizes[2], sizes[2], 1)
    return ep, tuple(ep // s % n for s, n in zip(strides, sizes)), strides


def greet_all(count):
    ep, tp = lax.axis_index("ep"), lax.axis_index("tp")
    barrier = pltpu.get_barrier_semaphore()

    def greet(k, carry):
        pl.semaphore_signal(
            barrier, inc=1, device_id=((ep + k) % count, tp), device_id_type=MESH
        )
        return carry

    lax.fori_loop(1, count, greet, 0)
    pl.semaphore_signal(barrier, inc=1, device_id=(ep, 1 - tp), device_id_type=MESH)
    pl.semaphore_wait(barrier, count)


def remote(src, dst, send, recv, device):
    return pltpu.make_async_remote_copy(
        src_ref=src,
        dst_ref=dst,
        send_sem=send,
        recv_sem=recv,
        device_id=device,
        device_id_type=MESH,
    )


def gather_kernel(
    sizes,
    partial,
    hidden,
    gain,
    meta,
    first,
    tokens,
    metas,
    sibling_part,
    part_sem,
    meta_send,
    meta_recv,
    send_sem,
    recv_sem,
    pass_send,
    pass_recv,
):
    count = sizes[0] * sizes[1] * sizes[2]
    ep, at, strides = position(sizes)
    tp = lax.axis_index("tp")
    half = first.shape[0]
    mine = pl.ds(pl.multiple_of(tp * half, half), half)
    other = pl.ds(pl.multiple_of((1 - tp) * half, half), half)
    greet_all(count)
    swap = remote(partial.at[other], sibling_part, part_sem.at[0], part_sem.at[1], (ep, 1 - tp))
    swap.start()

    def meta_copy(k):
        return remote(
            meta, metas.at[ep], meta_send.at[k], meta_recv.at[k], ((ep + k) % count, tp)
        )

    def start_meta(k, carry):
        meta_copy(k).start()
        return carry

    lax.fori_loop(1, count, start_meta, 0)
    metas[ep] = meta[...]
    swap.wait()
    total = (
        hidden[mine, :].astype(F32)
        + partial[mine, :].astype(F32)
        + sibling_part[...].astype(F32)
    ).astype(BF16)
    first[...] = total
    ffn_in = rms_scaled(total.astype(F32), gain[...]).astype(BF16)
    tokens[at[0], at[1], at[2], mine, :] = ffn_in

    def views(order, r):
        _, d2, d3 = order

        def view(k, second, third):
            spot = [pl.ds((at[0] + sizes[0] - k) % sizes[0], 1), None, None]
            spot[d2], spot[d3] = second, third
            return tokens.at[tuple(spot) + (r,)]

        def one(d, j=0):
            return pl.ds((at[d] + sizes[d] - j) % sizes[d], 1)

        whole = pl.ds(0, sizes[d2])
        return (
            lambda k, j=0: view(k, one(d2), one(d3)),
            lambda k, j=0: view(k, one(d2, j), one(d3)),
            lambda k, j=0: view(k, whole, one(d3, j)),
        )

    def run(core, order, order_of_other):
        sibling = (ep, 1 - core)
        come = views(order, pl.ds(core * half, half))
        chunks = sizes[0]
        flights, passed = {}, []

        def send(stage, k, j):
            d = order[stage]
            source = come[stage](0 if stage == 0 else k)
            peer = ep + ((at[d] + j) % sizes[d] - at[d]) * strides[d]
            slot = (stage, k, j if stage else 0)
            copy = remote(source, source, send_sem.at[slot], recv_sem.at[slot], (peer, core))
            copy.start()
            flights[slot] = copy

        def onward(stage, k, j):
            view = come[stage](k, j)
            slot = (stage, k, j)
            copy = remote(view, view, pass_send.at[slot], pass_recv.at[slot], sibling)
            copy.start()
            passed.append(copy)

        def first_phase(k):
            if k:
                flights[0, k, 0].wait()
            for j in range(1, sizes[order[1]]):
                send(1, k, j)
            onward(0, k, 0)

        def later_phase(stage, k):
            for j in range(1, sizes[order[stage]]):
                flights[stage, k, j].wait()
            if stage == 1:
                for j in range(1, sizes[order[2]]):
                    send(2, k, j)
            for j in range(1, sizes[order[stage]]):
                onward(stage, k, j)

        for k in range(1, chunks):
            send(0, k, k)
        for t in range(chunks + 2):
            if 0 <= t - 1 < chunks:
                later_phase(1, t - 1)
            if t < chunks:
                first_phase(t)
            if 0 <= t - 2 < chunks:
                later_phase(2, t - 2)
        for copy in passed:
            copy.wait_send()
        theirs = views(order_of_other, pl.ds((1 - core) * half, half))
        for stage in range(3):
            for k in range(chunks):
                for j in range(1, sizes[order_of_other[stage]]) if stage else (0,):
                    view, slot = theirs[stage](k, j), (stage, k, j)
                    remote(view, view, pass_send.at[slot], pass_recv.at[slot], sibling).wait_recv()

    @pl.when(tp == 0)
    def _():
        run(0, (0, 2, 1), (0, 1, 2))

    @pl.when(tp == 1)
    def _():
        run(1, (0, 1, 2), (0, 2, 1))

    def wait_meta(k, carry):
        meta_copy(k).wait()
        return carry

    lax.fori_loop(1, count, wait_meta, 0)


def gather_tokens(sizes, partial, hidden, gain, meta):
    seqs, width = hidden.shape
    count = sizes[0] * sizes[1] * sizes[2]
    half = seqs // 2
    most = max(sizes)
    dma = pltpu.SemaphoreType.DMA
    return pl.pallas_call(
        functools.partial(gather_kernel, sizes),
        out_shape=(
            jax.ShapeDtypeStruct((half, width), BF16),
            jax.ShapeDtypeStruct(sizes + (seqs, width), BF16),
            jax.ShapeDtypeStruct((count,) + meta.shape, F32),
        ),
        in_specs=[VMEM_SPEC] * 4,
        out_specs=(VMEM_SPEC,) * 3,
        scratch_shapes=[
            pltpu.VMEM((half, width), BF16),
            dma((2,)),
            dma((count,)),
            dma((count,)),
            dma((3, sizes[0], most)),
            dma((3, sizes[0], most)),
            dma((3, sizes[0], most)),
            dma((3, sizes[0], most)),
        ],
        compiler_params=pltpu.CompilerParams(
            collective_id=0, has_side_effects=True, vmem_limit_bytes=VMEM_LIMIT
        ),
        name="gather_tokens",
    )(partial, hidden, gain, meta)


def scatter_kernel(sizes, parts, first, out, total, from_sibling, land0, land1, sems):
    pair_send, pair_recv, send_sem, recv_sem, last_sem = sems
    ep, at, strides = position(sizes)
    tp = lax.axis_index("tp")
    half = first.shape[0]
    mine = pl.ds(pl.multiple_of(tp * half, half), half)
    other = pl.ds(pl.multiple_of((1 - tp) * half, half), half)
    chunks = sizes[0]
    goals = [(at[0] + 1 + k) % chunks for k in range(chunks)]
    greet_all(sizes[0] * sizes[1] * sizes[2])
    pairs = []
    for k in range(chunks):
        copy = remote(
            parts.at[goals[k], :, :, other],
            from_sibling.at[k],
            pair_send.at[k],
            pair_recv.at[k],
            (ep, 1 - tp),
        )
        copy.start()
        pairs.append(copy)

    def run(core, d1, d2, lands):
        rows = pl.ds(core * half, half)
        flights = {}

        def spot(k, c1, c2):
            place = [goals[k], None, None]
            place[d1], place[d2] = c1, c2
            return tuple(place)

        def send(stage, k, j, source, dst, d):
            peer = ep + ((at[d] + j) % sizes[d] - at[d]) * strides[d]
            slot = (stage, k, j if stage < 2 else 0)
            copy = remote(source, dst, send_sem.at[slot], recv_sem.at[slot], (peer, core))
            copy.start()
            flights[slot] = copy

        def pair_sum(k):
            pairs[k].wait()

            def add(b, carry):
                y, x = b // sizes[2], b % sizes[2]
                total[goals[k], y, x] = (
                    parts[goals[k], y, x, rows, :].astype(F32) + from_sibling[k, y, x].astype(F32)
                ).astype(BF16)
                return carry

            lax.fori_loop(0, sizes[1] * sizes[2], add, 0)
            for j in range(1, sizes[d1]):
                source = total.at[spot(k, (at[d1] + j) % sizes[d1], slice(None))]
                send(0, k, j, source, lands[0].at[k, j - 1], d1)

        def first_sum(k):
            for j in range(1, sizes[d1]):
                flights[0, k, j].wait()

            def add(b, carry):
                place = spot(k, at[d1], b)
                value = total[place].astype(F32)
                for j in range(1, sizes[d1]):
                    value = value + lands[0][k, j - 1, b].astype(F32)
                total[place] = value.astype(BF16)
                return carry

            lax.fori_loop(0, sizes[d2], add, 0)
            for j in range(1, sizes[d2]):
                source = total.at[spot(k, at[d1], (at[d2] + j) % sizes[d2])]
                send(1, k, j, source, lands[1].at[k, j - 1], d2)

        def second_sum(k):
            for j in range(1, sizes[d2]):
                flights[1, k, j].wait()
            place = spot(k, at[d1], at[d2])
            value = total[place].astype(F32)
            for j in range(1, sizes[d2]):
                value = value + lands[1][k, j - 1].astype(F32)
            if k < chunks - 1:
                total[place] = value.astype(BF16)
                send(2, k, k + 1, total.at[place], lands[2].at[k], 0)
                return
            value = value + first[...].astype(F32)
            for i in range(chunks - 1):
                flights[2, i, 0].wait()
                value = value + lands[2][i].astype(F32)
            out[rows, :] = value.astype(BF16)

        for t in range(chunks + 2):
            if t < chunks:
                pair_sum(t)
            if 0 <= t - 1 < chunks:
                first_sum(t - 1)
            if 0 <= t - 2 < chunks:
                second_sum(t - 2)

    @pl.when(tp == 0)
    def _():
        run(0, 1, 2, land0)

    @pl.when(tp == 1)
    def _():
        run(1, 2, 1, land1)

    swap = remote(out.at[mine], out.at[mine], last_sem.at[0], last_sem.at[1], (ep, 1 - tp))
    swap.start()
    swap.wait()


def landing(sizes, d1, d2, half, width):
    chunks, block = sizes[0], (half, width)
    return [
        pltpu.VMEM((chunks, max(1, sizes[d1] - 1), sizes[d2]) + block, BF16),
        pltpu.VMEM((chunks, max(1, sizes[d2] - 1)) + block, BF16),
        pltpu.VMEM((max(1, chunks - 1),) + block, BF16),
    ]


def scatter_sum(sizes, parts, first):
    half, width = first.shape
    most = max(sizes)
    dma = pltpu.SemaphoreType.DMA
    return pl.pallas_call(
        functools.partial(scatter_kernel, sizes),
        out_shape=jax.ShapeDtypeStruct((2 * half, width), BF16),
        in_specs=[VMEM_SPEC] * 2,
        out_specs=VMEM_SPEC,
        scratch_shapes=[
            pltpu.VMEM(sizes + (half, width), BF16),
            pltpu.VMEM(sizes + (half, width), BF16),
            landing(sizes, 1, 2, half, width),
            landing(sizes, 2, 1, half, width),
            [
                dma((sizes[0],)),
                dma((sizes[0],)),
                dma((3, sizes[0], most)),
                dma((3, sizes[0], most)),
                dma((2,)),
            ],
        ],
        compiler_params=pltpu.CompilerParams(
            collective_id=1, has_side_effects=True, vmem_limit_bytes=VMEM_LIMIT
        ),
        name="scatter_sum",
    )(parts, first)


def shards(
    hidden,
    mix_gain,
    recept_weight,
    key_weight,
    value_weight,
    decay_down,
    decay_up,
    decay_bias,
    rate_down,
    rate_up,
    rate_bias,
    head_gain,
    out_weight,
    memory_state,
    ffn_gain,
    blend_vector,
    dense_gate,
    dense_up,
    dense_down,
    expert_gate,
    expert_up,
    expert_down,
    routing,
    route_scale,
):
    seqs, width = hidden.shape
    count = lax.axis_size("ep")
    sizes = factors_of(count)
    top = routing.shape[1]
    cap = max(2, 2 * seqs * top // count)
    new_state, partial = attention(
        hidden,
        (
            mix_gain[None],
            recept_weight,
            key_weight,
            value_weight,
            decay_down.T,
            decay_up,
            decay_bias[None],
            rate_down.T,
            rate_up,
            rate_bias[None],
            head_gain[None],
            out_weight,
        ),
        memory_state,
    )
    meta = jnp.concatenate([routing.T.astype(F32), route_scale.T], axis=0)
    meta = jnp.pad(meta, ((0, -2 * top % 8), (0, -seqs % 128)))
    first, tokens, metas = gather_tokens(sizes, partial, hidden, ffn_gain[None], meta)
    tokens = tokens.reshape(count * seqs, width)

    hit = metas[:, :top, :seqs] == lax.axis_index("ep").astype(F32)
    chosen = jnp.any(hit, axis=1)
    scale_of = jnp.sum(jnp.where(hit, metas[:, top : 2 * top, :seqs], 0.0), axis=1)
    earlier = jnp.arange(seqs)[:, None] < jnp.arange(seqs)[None, :]
    rank = matmul(chosen.astype(BF16), earlier.astype(BF16)).astype(jnp.int32)
    place = jnp.where(chosen, rank + jnp.arange(count, dtype=jnp.int32)[:, None] * cap, -1)
    select = place.reshape(1, -1) == jnp.arange(count * cap, dtype=jnp.int32)[:, None]
    slot_scale = jnp.sum(jnp.where(select, scale_of.reshape(1, -1), 0.0), axis=1, keepdims=True)
    picked = matmul(select.astype(BF16), tokens).astype(BF16)
    expert_act = (silu_of(matmul(picked, expert_gate[0])) * matmul(picked, expert_up[0])).astype(BF16)
    expert_out = (matmul(expert_act, expert_down[0]) * slot_scale).astype(BF16)
    blend = jax.nn.sigmoid(matmul_nt(tokens, blend_vector[None]))
    dense_act = (
        silu_of(matmul(tokens, dense_gate)) * matmul(tokens, dense_up) * blend
    ).astype(BF16)
    spread = (place.reshape(-1, 1) == jnp.arange(count * cap, dtype=jnp.int32)[None, :]).astype(BF16)
    parts = matmul(
        jnp.concatenate([spread, dense_act], axis=1),
        jnp.concatenate([expert_out, dense_down], axis=0),
    ).astype(BF16)
    layer_out = scatter_sum(sizes, parts.reshape(sizes + (seqs, width)), first)
    return (layer_out, new_state)


def solution(mesh):
    in_specs = (
        P("ep", None),
        P(),
        P(None, "tp"),
        P(None, "tp"),
        P(None, "tp"),
        P(),
        P(),
        P(),
        P(),
        P(),
        P(),
        P(),
        P("tp", None),
        P("ep", "tp", None, None),
        P(),
        P(),
        P(None, ("ep", "tp")),
        P(None, ("ep", "tp")),
        P(("ep", "tp"), None),
        P("ep", None, "tp"),
        P("ep", None, "tp"),
        P("ep", "tp", None),
        P("ep", None),
        P("ep", None),
    )
    out_specs = (P("ep", None), P("ep", "tp", None, None))
    return jax.shard_map(shards, mesh=mesh, in_specs=in_specs, out_specs=out_specs, check_vma=False)
```

```python
import functools
import math

import jax
import jax.numpy as jnp
from jax import lax
from jax.experimental import pallas as pl
from jax.experimental.pallas import tpu as pltpu
from jax.sharding import PartitionSpec as P

MESH = pl.DeviceIdType.MESH
F32 = jnp.float32
BF16 = jnp.bfloat16
VMEM_LIMIT = 64 * 1024 * 1024 - 65536
VMEM_SPEC = pl.BlockSpec(memory_space=pltpu.VMEM)


def matmul(left, right):
    return jnp.dot(left, right, preferred_element_type=F32)


def matmul_nt(left, right):
    return lax.dot_general(left, right, (((1,), (1,)), ((), ())), preferred_element_type=F32)


def silu_of(tensor):
    return tensor / (1.0 + jnp.exp(-tensor))


def rms_scaled(values, gain):
    return values * lax.rsqrt(jnp.mean(values * values, axis=-1, keepdims=True) + 1e-06) * gain


def factors_of(count):
    slow = 4 if count % 4 == 0 else 1
    rest = count // slow
    mid = math.isqrt(rest)
    while rest % mid:
        mid -= 1
    return slow, mid, rest // mid


def attention_kernel(
    step_rows,
    hidden,
    mix_gain,
    recept_weight,
    key_weight,
    value_weight,
    decay_down,
    decay_up,
    decay_bias,
    rate_down,
    rate_up,
    rate_bias,
    head_gain,
    out_weight,
    state_in,
    state_out,
    partial,
    recept_s,
    unit_s,
    unit_rate_s,
    key_rate_s,
    value_s,
    decay_s,
    readout_s,
    normed_s,
):
    step = pl.program_id(0)
    heads, seqs, size = recept_s.shape
    width = heads * size
    own = pl.ds(pl.multiple_of(lax.axis_index("tp") * width, 128), width)

    @pl.when(step == 0)
    def _():
        normed = rms_scaled(hidden[...].astype(F32), mix_gain[...]).astype(BF16)
        recept = matmul(normed, recept_weight[...]).astype(BF16).astype(F32)
        keys = matmul(normed, key_weight[...]).astype(BF16).astype(F32)
        vals = matmul(normed, value_weight[...]).astype(BF16).astype(F32)
        decay_low = jnp.tanh(matmul_nt(normed, decay_down[...])).astype(BF16)
        decay_pre = matmul(decay_low, decay_up[:, own]) + decay_bias[:, own]
        softplus = jnp.maximum(-decay_pre, 0.0) + jnp.log1p(jnp.exp(-jnp.abs(decay_pre)))
        decay = jnp.exp(-jnp.exp(-softplus - 0.5))
        rate_low = matmul_nt(normed, rate_down[...]).astype(BF16)
        rate = 1.0 / (1.0 + jnp.exp(-(matmul(rate_low, rate_up[:, own]) + rate_bias[:, own])))
        for h in range(heads):
            cols = slice(h * size, (h + 1) * size)
            key_h, rate_h = keys[:, cols], rate[:, cols]
            unit = key_h * lax.rsqrt(jnp.sum(key_h * key_h, axis=-1, keepdims=True) + 1e-06)
            recept_s[h] = recept[:, cols]
            unit_s[h] = unit
            unit_rate_s[h] = unit * rate_h
            key_rate_s[h] = key_h * rate_h
            value_s[h] = vals[:, cols]
            decay_s[h] = decay[:, cols]

    shape, flat = (heads, size, size), (heads * size, size)
    eye = lax.broadcasted_iota(jnp.int32, shape, 1) == lax.broadcasted_iota(jnp.int32, shape, 2)
    ones = jnp.ones((size, size), BF16)

    def row_sums(values):
        return matmul(values.astype(BF16).reshape(flat), ones).reshape(shape)

    def one_sequence(local, carry):
        row = pl.ds(step * step_rows + local, 1)
        state = state_in[local]
        removed = row_sums(state * unit_s[:, row])
        value = row_sums(jnp.where(eye, value_s[:, row], 0.0))
        new = (
            state * decay_s[:, row] - removed * unit_rate_s[:, row] + value * key_rate_s[:, row]
        )
        state_out[local] = new
        out = row_sums(new * recept_s[:, row])
        readout_s[:, row] = jnp.sum(jnp.where(eye, out, 0.0), axis=1, keepdims=True)
        return carry

    lax.fori_loop(0, step_rows, one_sequence, 0, unroll=4)

    @pl.when(step == pl.num_programs(0) - 1)
    def _():
        gain = head_gain[:, own]
        for h in range(heads):
            cols = slice(h * size, (h + 1) * size)
            out = readout_s[h]
            centred = out - jnp.mean(out, axis=-1, keepdims=True)
            variance = jnp.mean(centred * centred, axis=-1, keepdims=True)
            normed_s[:, cols] = (centred * lax.rsqrt(variance + 0.00064) * gain[:, cols]).astype(BF16)
        partial[...] = matmul(normed_s[...], out_weight[...]).astype(BF16)


def attention(hidden, vectors, state):
    seqs, heads, size, _ = state.shape
    width = heads * size
    step_rows = math.gcd(seqs, 8)
    block = pl.BlockSpec((step_rows, heads, size, size), lambda i: (i, 0, 0, 0))
    operands = (hidden,) + vectors
    whole = [pl.BlockSpec(a.shape, lambda i: (0, 0)) for a in operands]
    per_head = pltpu.VMEM((heads, seqs, size), F32)
    return pl.pallas_call(
        functools.partial(attention_kernel, step_rows),
        grid=(seqs // step_rows,),
        out_shape=(
            jax.ShapeDtypeStruct(state.shape, F32),
            jax.ShapeDtypeStruct(hidden.shape, BF16),
        ),
        in_specs=whole + [block],
        out_specs=(block, pl.BlockSpec(hidden.shape, lambda i: (0, 0))),
        scratch_shapes=[per_head] * 7 + [pltpu.VMEM((seqs, width), BF16)],
        compiler_params=pltpu.CompilerParams(
            dimension_semantics=("arbitrary",), vmem_limit_bytes=VMEM_LIMIT
        ),
        name="attention",
    )(*operands, state)


def position(sizes):
    ep = lax.axis_index("ep")
    strides = (sizes[1] * sizes[2], sizes[2], 1)
    return ep, tuple(ep // s % n for s, n in zip(strides, sizes)), strides


def greet_all(count):
    ep, tp = lax.axis_index("ep"), lax.axis_index("tp")
    barrier = pltpu.get_barrier_semaphore()

    def greet(k, carry):
        pl.semaphore_signal(
            barrier, inc=1, device_id=((ep + k) % count, tp), device_id_type=MESH
        )
        return carry

    lax.fori_loop(1, count, greet, 0)
    pl.semaphore_signal(barrier, inc=1, device_id=(ep, 1 - tp), device_id_type=MESH)
    pl.semaphore_wait(barrier, count)


def remote(src, dst, send, recv, device):
    return pltpu.make_async_remote_copy(
        src_ref=src,
        dst_ref=dst,
        send_sem=send,
        recv_sem=recv,
        device_id=device,
        device_id_type=MESH,
    )


def gather_kernel(
    sizes,
    partial,
    hidden,
    gain,
    meta,
    first,
    tokens,
    metas,
    sibling_part,
    part_sem,
    meta_send,
    meta_recv,
    send_sem,
    recv_sem,
    pass_send,
    pass_recv,
):
    count = sizes[0] * sizes[1] * sizes[2]
    ep, at, strides = position(sizes)
    tp = lax.axis_index("tp")
    half = first.shape[0]
    mine = pl.ds(pl.multiple_of(tp * half, half), half)
    other = pl.ds(pl.multiple_of((1 - tp) * half, half), half)
    greet_all(count)
    swap = remote(partial.at[other], sibling_part, part_sem.at[0], part_sem.at[1], (ep, 1 - tp))
    swap.start()

    def meta_copy(k):
        return remote(
            meta, metas.at[ep], meta_send.at[k], meta_recv.at[k], ((ep + k) % count, tp)
        )

    def start_meta(k, carry):
        meta_copy(k).start()
        return carry

    lax.fori_loop(1, count, start_meta, 0)
    metas[ep] = meta[...]
    swap.wait()
    total = (
        hidden[mine, :].astype(F32)
        + partial[mine, :].astype(F32)
        + sibling_part[...].astype(F32)
    ).astype(BF16)
    first[...] = total
    ffn_in = rms_scaled(total.astype(F32), gain[...]).astype(BF16)
    tokens[at[0], at[1], at[2], mine, :] = ffn_in

    def views(order, r):
        _, d2, d3 = order

        def view(k, second, third):
            spot = [pl.ds((at[0] + sizes[0] - k) % sizes[0], 1), None, None]
            spot[d2], spot[d3] = second, third
            return tokens.at[tuple(spot) + (r,)]

        def one(d, j=0):
            return pl.ds((at[d] + sizes[d] - j) % sizes[d], 1)

        whole = pl.ds(0, sizes[d2])
        return (
            lambda k, j=0: view(k, one(d2), one(d3)),
            lambda k, j=0: view(k, one(d2, j), one(d3)),
            lambda k, j=0: view(k, whole, one(d3, j)),
        )

    def run(core, order, order_of_other):
        sibling = (ep, 1 - core)
        come = views(order, pl.ds(core * half, half))
        chunks = sizes[0]
        flights, passed = {}, []

        def send(stage, k, j):
            d = order[stage]
            source = come[stage](0 if stage == 0 else k)
            peer = ep + ((at[d] + j) % sizes[d] - at[d]) * strides[d]
            slot = (stage, k, j if stage else 0)
            copy = remote(source, source, send_sem.at[slot], recv_sem.at[slot], (peer, core))
            copy.start()
            flights[slot] = copy

        def onward(stage, k, j):
            view = come[stage](k, j)
            slot = (stage, k, j)
            copy = remote(view, view, pass_send.at[slot], pass_recv.at[slot], sibling)
            copy.start()
            passed.append(copy)

        def first_phase(k):
            if k:
                flights[0, k, 0].wait()
            for j in range(1, sizes[order[1]]):
                send(1, k, j)
            onward(0, k, 0)

        def later_phase(stage, k):
            for j in range(1, sizes[order[stage]]):
                flights[stage, k, j].wait()
            if stage == 1:
                for j in range(1, sizes[order[2]]):
                    send(2, k, j)
            for j in range(1, sizes[order[stage]]):
                onward(stage, k, j)

        first_phase(0)
        for k in range(1, chunks):
            send(0, k, k)
        for t in range(chunks + 2):
            if 0 <= t - 1 < chunks:
                later_phase(1, t - 1)
            if 0 < t < chunks:
                first_phase(t)
            if 0 <= t - 2 < chunks:
                later_phase(2, t - 2)
        for copy in passed:
            copy.wait_send()
        theirs = views(order_of_other, pl.ds((1 - core) * half, half))
        for stage in range(3):
            for k in range(chunks):
                for j in range(1, sizes[order_of_other[stage]]) if stage else (0,):
                    view, slot = theirs[stage](k, j), (stage, k, j)
                    remote(view, view, pass_send.at[slot], pass_recv.at[slot], sibling).wait_recv()

    @pl.when(tp == 0)
    def _():
        run(0, (0, 2, 1), (0, 1, 2))

    @pl.when(tp == 1)
    def _():
        run(1, (0, 1, 2), (0, 2, 1))

    def wait_meta(k, carry):
        meta_copy(k).wait()
        return carry

    lax.fori_loop(1, count, wait_meta, 0)


def gather_tokens(sizes, partial, hidden, gain, meta):
    seqs, width = hidden.shape
    count = sizes[0] * sizes[1] * sizes[2]
    half = seqs // 2
    most = max(sizes)
    dma = pltpu.SemaphoreType.DMA
    return pl.pallas_call(
        functools.partial(gather_kernel, sizes),
        out_shape=(
            jax.ShapeDtypeStruct((half, width), BF16),
            jax.ShapeDtypeStruct(sizes + (seqs, width), BF16),
            jax.ShapeDtypeStruct((count,) + meta.shape, F32),
        ),
        in_specs=[VMEM_SPEC] * 4,
        out_specs=(VMEM_SPEC,) * 3,
        scratch_shapes=[
            pltpu.VMEM((half, width), BF16),
            dma((2,)),
            dma((count,)),
            dma((count,)),
            dma((3, sizes[0], most)),
            dma((3, sizes[0], most)),
            dma((3, sizes[0], most)),
            dma((3, sizes[0], most)),
        ],
        compiler_params=pltpu.CompilerParams(
            collective_id=0, has_side_effects=True, vmem_limit_bytes=VMEM_LIMIT
        ),
        name="gather_tokens",
    )(partial, hidden, gain, meta)


def scatter_kernel(sizes, parts, first, out, total, from_sibling, land0, land1, sems):
    pair_send, pair_recv, send_sem, recv_sem, last_sem = sems
    ep, at, strides = position(sizes)
    tp = lax.axis_index("tp")
    half = first.shape[0]
    mine = pl.ds(pl.multiple_of(tp * half, half), half)
    other = pl.ds(pl.multiple_of((1 - tp) * half, half), half)
    chunks = sizes[0]
    goals = [(at[0] + 1 + k) % chunks for k in range(chunks)]
    greet_all(sizes[0] * sizes[1] * sizes[2])
    pairs = []
    for k in range(chunks):
        copy = remote(
            parts.at[goals[k], :, :, other],
            from_sibling.at[k],
            pair_send.at[k],
            pair_recv.at[k],
            (ep, 1 - tp),
        )
        copy.start()
        pairs.append(copy)

    def run(core, d1, d2, lands):
        rows = pl.ds(core * half, half)
        flights = {}

        def spot(k, c1, c2):
            place = [goals[k], None, None]
            place[d1], place[d2] = c1, c2
            return tuple(place)

        def send(stage, k, j, source, dst, d):
            peer = ep + ((at[d] + j) % sizes[d] - at[d]) * strides[d]
            slot = (stage, k, j if stage < 2 else 0)
            copy = remote(source, dst, send_sem.at[slot], recv_sem.at[slot], (peer, core))
            copy.start()
            flights[slot] = copy

        def pair_sum(k):
            pairs[k].wait()

            def add(b, carry):
                y, x = b // sizes[2], b % sizes[2]
                total[goals[k], y, x] = (
                    parts[goals[k], y, x, rows, :].astype(F32) + from_sibling[k, y, x].astype(F32)
                ).astype(BF16)
                return carry

            lax.fori_loop(0, sizes[1] * sizes[2], add, 0)
            for j in range(1, sizes[d1]):
                source = total.at[spot(k, (at[d1] + j) % sizes[d1], slice(None))]
                send(0, k, j, source, lands[0].at[k, j - 1], d1)

        def first_sum(k):
            for j in range(1, sizes[d1]):
                flights[0, k, j].wait()

            def add(b, carry):
                place = spot(k, at[d1], b)
                value = total[place].astype(F32)
                for j in range(1, sizes[d1]):
                    value = value + lands[0][k, j - 1, b].astype(F32)
                total[place] = value.astype(BF16)
                return carry

            lax.fori_loop(0, sizes[d2], add, 0)
            for j in range(1, sizes[d2]):
                source = total.at[spot(k, at[d1], (at[d2] + j) % sizes[d2])]
                send(1, k, j, source, lands[1].at[k, j - 1], d2)

        def second_sum(k):
            for j in range(1, sizes[d2]):
                flights[1, k, j].wait()
            place = spot(k, at[d1], at[d2])
            value = total[place].astype(F32)
            for j in range(1, sizes[d2]):
                value = value + lands[1][k, j - 1].astype(F32)
            if k < chunks - 1:
                total[place] = value.astype(BF16)
                send(2, k, k + 1, total.at[place], lands[2].at[k], 0)
                return
            value = value + first[...].astype(F32)
            for i in range(chunks - 1):
                flights[2, i, 0].wait()
                value = value + lands[2][i].astype(F32)
            out[rows, :] = value.astype(BF16)

        for t in range(chunks + 2):
            if t < chunks:
                pair_sum(t)
            if 0 <= t - 1 < chunks:
                first_sum(t - 1)
            if 0 <= t - 2 < chunks:
                second_sum(t - 2)

    @pl.when(tp == 0)
    def _():
        run(0, 1, 2, land0)

    @pl.when(tp == 1)
    def _():
        run(1, 2, 1, land1)

    swap = remote(out.at[mine], out.at[mine], last_sem.at[0], last_sem.at[1], (ep, 1 - tp))
    swap.start()
    swap.wait()


def landing(sizes, d1, d2, half, width):
    chunks, block = sizes[0], (half, width)
    return [
        pltpu.VMEM((chunks, max(1, sizes[d1] - 1), sizes[d2]) + block, BF16),
        pltpu.VMEM((chunks, max(1, sizes[d2] - 1)) + block, BF16),
        pltpu.VMEM((max(1, chunks - 1),) + block, BF16),
    ]


def scatter_sum(sizes, parts, first):
    half, width = first.shape
    most = max(sizes)
    dma = pltpu.SemaphoreType.DMA
    return pl.pallas_call(
        functools.partial(scatter_kernel, sizes),
        out_shape=jax.ShapeDtypeStruct((2 * half, width), BF16),
        in_specs=[VMEM_SPEC] * 2,
        out_specs=VMEM_SPEC,
        scratch_shapes=[
            pltpu.VMEM(sizes + (half, width), BF16),
            pltpu.VMEM(sizes + (half, width), BF16),
            landing(sizes, 1, 2, half, width),
            landing(sizes, 2, 1, half, width),
            [
                dma((sizes[0],)),
                dma((sizes[0],)),
                dma((3, sizes[0], most)),
                dma((3, sizes[0], most)),
                dma((2,)),
            ],
        ],
        compiler_params=pltpu.CompilerParams(
            collective_id=1, has_side_effects=True, vmem_limit_bytes=VMEM_LIMIT
        ),
        name="scatter_sum",
    )(parts, first)


def shards(
    hidden,
    mix_gain,
    recept_weight,
    key_weight,
    value_weight,
    decay_down,
    decay_up,
    decay_bias,
    rate_down,
    rate_up,
    rate_bias,
    head_gain,
    out_weight,
    memory_state,
    ffn_gain,
    blend_vector,
    dense_gate,
    dense_up,
    dense_down,
    expert_gate,
    expert_up,
    expert_down,
    routing,
    route_scale,
):
    seqs, width = hidden.shape
    count = lax.axis_size("ep")
    sizes = factors_of(count)
    top = routing.shape[1]
    cap = max(2, 2 * seqs * top // count)
    new_state, partial = attention(
        hidden,
        (
            mix_gain[None],
            recept_weight,
            key_weight,
            value_weight,
            decay_down.T,
            decay_up,
            decay_bias[None],
            rate_down.T,
            rate_up,
            rate_bias[None],
            head_gain[None],
            out_weight,
        ),
        memory_state,
    )
    meta = jnp.concatenate([routing.T.astype(F32), route_scale.T], axis=0)
    meta = jnp.pad(meta, ((0, -2 * top % 8), (0, -seqs % 128)))
    first, tokens, metas = gather_tokens(sizes, partial, hidden, ffn_gain[None], meta)
    tokens = tokens.reshape(count * seqs, width)

    hit = metas[:, :top, :seqs] == lax.axis_index("ep").astype(F32)
    chosen = jnp.any(hit, axis=1)
    scale_of = jnp.sum(jnp.where(hit, metas[:, top : 2 * top, :seqs], 0.0), axis=1)
    earlier = jnp.arange(seqs)[:, None] < jnp.arange(seqs)[None, :]
    rank = matmul(chosen.astype(BF16), earlier.astype(BF16)).astype(jnp.int32)
    place = jnp.where(chosen, rank + jnp.arange(count, dtype=jnp.int32)[:, None] * cap, -1)
    select = place.reshape(1, -1) == jnp.arange(count * cap, dtype=jnp.int32)[:, None]
    slot_scale = jnp.sum(jnp.where(select, scale_of.reshape(1, -1), 0.0), axis=1, keepdims=True)
    picked = matmul(select.astype(BF16), tokens).astype(BF16)
    expert_act = (silu_of(matmul(picked, expert_gate[0])) * matmul(picked, expert_up[0])).astype(BF16)
    expert_out = (matmul(expert_act, expert_down[0]) * slot_scale).astype(BF16)
    blend = jax.nn.sigmoid(matmul_nt(tokens, blend_vector[None]))
    dense_act = (
        silu_of(matmul(tokens, dense_gate)) * matmul(tokens, dense_up) * blend
    ).astype(BF16)
    spread = (place.reshape(-1, 1) == jnp.arange(count * cap, dtype=jnp.int32)[None, :]).astype(BF16)
    parts = matmul(
        jnp.concatenate([spread, dense_act], axis=1),
        jnp.concatenate([expert_out, dense_down], axis=0),
    ).astype(BF16)
    layer_out = scatter_sum(sizes, parts.reshape(sizes + (seqs, width)), first)
    return (layer_out, new_state)


def solution(mesh):
    in_specs = (
        P("ep", None),
        P(),
        P(None, "tp"),
        P(None, "tp"),
        P(None, "tp"),
        P(),
        P(),
        P(),
        P(),
        P(),
        P(),
        P(),
        P("tp", None),
        P("ep", "tp", None, None),
        P(),
        P(),
        P(None, ("ep", "tp")),
        P(None, ("ep", "tp")),
        P(("ep", "tp"), None),
        P("ep", None, "tp"),
        P("ep", None, "tp"),
        P("ep", "tp", None),
        P("ep", None),
        P("ep", None),
    )
    out_specs = (P("ep", None), P("ep", "tp", None, None))
    return jax.shard_map(shards, mesh=mesh, in_specs=in_specs, out_specs=out_specs, check_vma=False)
```
